32 devices in a mesh: kv: 8 (over z, x), tp: 4 (over y, core).
Axes of the slice: x: 2, y: 2, z: 4, core: 2. Of those that a mesh axis runs over, the one named last changes fastest.
Arguments:
- tokens: bfloat16 [22, 4096], P(None, ('kv', 'tp')), may hold values from -22 to 22
- attn_gain: float32 [4096], P('kv'), may hold values from 0.1 to 1.9
- w_query: bfloat16 [4096, 4096], P('kv', 'tp'), may hold values from -0.09375 to 0.09375
- w_key: bfloat16 [4096, 4096], P('kv', 'tp'), may hold values from -0.5 to 0.5
- w_value: bfloat16 [4096, 4096], P('kv', 'tp'), may hold values from -0.09375 to 0.09375
- cache_keys: bfloat16 [22, 2048, 32, 128], P(None, 'kv', 'tp'), may hold values from -256 to 256
- cache_values: bfloat16 [22, 2048, 32, 128], P(None, 'kv', 'tp'), may hold values from -6 to 6
- lambdas: float32 [32], P('tp'), may hold values from 0.3 to 0.8
- head_gain: float32 [128], replicated, may hold values from 0.1 to 1.9
- w_out: bfloat16 [4096, 4096], P('tp', 'kv'), may hold values from -0.09375 to 0.09375
- mlp_gain: float32 [4096], P('kv'), may hold values from 0.1 to 1.9
- w_gate: bfloat16 [4096, 11008], P('kv', 'tp'), may hold values from -0.09375 to 0.09375
- w_up: bfloat16 [4096, 11008], P('kv', 'tp'), may hold values from -0.09375 to 0.09375
- w_down: bfloat16 [11008, 4096], P('tp', 'kv'), may hold values from -0.0546875 to 0.0546875
Outputs:
- output: bfloat16 [22, 4096], P(None, ('kv', 'tp'))
The draws below stay inside these ranges and needn't reach their ends.
All inputs are finite; a program needn't handle non-finite values.
Results may differ from the reference program's by a relative error of at most 0.017.
The reference program's roundings to bfloat16 on the way (of `normed_in`, `query_all`, `heads_out`, `residual`, `normed_mid` and `hidden`) count: a program that leaves them out, or rounds other values in their place, can miss the bound.
Values may be sent and summed in bfloat16 or wider, within the bound.
A program may use at most 128 MiB of HBM per device.

```python
import jax
import jax.numpy as jnp
from jax import lax

D = 4096
HEADS = 32
HEAD_DIM = 128
HALF = 64
FF = 11008
SEQS = 22
POS_DEV = 256
CACHE_LEN = 2048
N_KV = 8
N_TP = 4


def draw_tokens(key, part):
    key_base = jax.random.fold_in(key, 11)
    key_rows = jax.random.fold_in(key, 12)
    columns = jnp.arange(D, dtype=jnp.float32) / (D - 1)
    base_vals = jnp.clip(jax.random.normal(key_base, (SEQS, D), jnp.float32), -4.0, 4.0)
    col_scale = jnp.exp(jnp.log(3.0) * (columns - 0.5))
    row_scale = jnp.exp(jax.random.uniform(key_rows, (SEQS, 1), jnp.float32, jnp.log(1.0 / 3.0), jnp.log(3.0)))
    return (base_vals * row_scale * col_scale[None, :]).astype(jnp.bfloat16)


def draw_cache_keys(key, part):
    key_base = jax.random.fold_in(key, 21)
    base_vals = jnp.clip(jax.random.normal(key_base, (SEQS, CACHE_LEN, HEADS, HEAD_DIM), jnp.float32), -6.0, 6.0) * 1.75
    return base_vals.astype(jnp.bfloat16)


def block_levels(rng, shape, cuts, low, high):
    loudness, own = 1.0, jax.random.fold_in(rng, 6)
    for axis_at, blocks in cuts:
        steps = jnp.exp(jax.random.uniform(jax.random.fold_in(own, axis_at), (blocks,), jnp.float32, low / len(cuts), high / len(cuts)))
        loudness = loudness * jnp.repeat(steps, shape[axis_at] // blocks).reshape([-1 if axis == axis_at else 1 for axis in range(len(shape))])
    return loudness


def bell_draw(key, dims, spread, bound, split=(), kind=jnp.bfloat16):
    level = block_levels(key, dims, split, -0.22, 0.18) if split else 1.0
    entries = jax.random.normal(key, dims, jnp.float32) * spread * level
    return jnp.minimum(jnp.maximum(entries, -bound), bound).astype(kind)


def setup_inputs(seed: int = 0) -> dict:
    key_of = jax.random.split(jax.random.key(seed), 15)
    tokens = draw_tokens(jax.random.fold_in(key_of[14], 71), 0)
    attn_gain = jnp.clip(1.0 + 0.18 * jax.random.normal(key_of[1], (D,), jnp.float32), 0.1, 1.9)
    w_query = bell_draw(key_of[2], (D, HEADS * HEAD_DIM), D ** -0.5, 0.09375, ((0, 8), (1, 4)))
    w_key = bell_draw(key_of[3], (D, HEADS * HEAD_DIM), (D // 36) ** -0.5, 0.5, ((0, 8), (1, 4)))
    w_value = bell_draw(key_of[4], (D, HEADS * HEAD_DIM), D ** -0.5, 0.09375, ((0, 8), (1, 4)))
    cache_keys = draw_cache_keys(jax.random.fold_in(key_of[14], 71), 0)
    cache_values = bell_draw(key_of[6], (SEQS, CACHE_LEN, HEADS, HEAD_DIM), 1.0, 6.0, ((1, 8), (2, 4)))
    lambdas = jnp.clip(0.3 + 0.5 * jax.random.uniform(key_of[7], (HEADS,), jnp.float32) ** block_levels(key_of[7], (HEADS,), ((0, 4),), -0.2, 0.2), 0.3, 0.8)
    head_gain = jnp.clip(1.0 + 0.18 * jax.random.normal(key_of[8], (HEAD_DIM,), jnp.float32), 0.1, 1.9)
    w_out = bell_draw(key_of[9], (HEADS * HEAD_DIM, D), (HEADS * HEAD_DIM) ** -0.5, 0.09375, ((0, 4), (1, 8)))
    mlp_gain = jnp.clip(1.0 + 0.18 * jax.random.normal(key_of[10], (D,), jnp.float32), 0.1, 1.9)
    w_gate = bell_draw(key_of[11], (D, FF), D ** -0.5, 0.09375, ((0, 8), (1, 4)))
    w_up = bell_draw(key_of[12], (D, FF), D ** -0.5, 0.09375, ((0, 8), (1, 4)))
    w_down = bell_draw(key_of[13], (FF, D), FF ** -0.5, 0.0546875, ((0, 4), (1, 8)))
    return dict(tokens=tokens, attn_gain=attn_gain, w_query=w_query, w_key=w_key, w_value=w_value, cache_keys=cache_keys, cache_values=cache_values, lambdas=lambdas, head_gain=head_gain, w_out=w_out, mlp_gain=mlp_gain, w_gate=w_gate, w_up=w_up, w_down=w_down)


epsilon = 1e-06

def blocked_attention(query_vec, key_new, value_new, keys_head, values_head, low, high):
    seq_count = keys_head.shape[0]
    score_scale = HALF ** (-0.5)
    query_part = query_vec[:, low:high].astype(jnp.float32)
    scores = jnp.einsum('sd,std->st', query_part, keys_head[:, :, low:high].astype(jnp.float32)) * score_scale
    score_new = lax.optimization_barrier(jnp.sum(query_part * key_new[:, low:high].astype(jnp.float32), axis=1)) * score_scale
    blocks = scores.reshape(seq_count, N_KV, POS_DEV)
    maxima = lax.optimization_barrier(jnp.max(blocks, axis=2))
    weights = jnp.exp(blocks - maxima[:, :, None])
    totals = lax.optimization_barrier(jnp.sum(weights, axis=2))
    rounded = lax.optimization_barrier(weights.astype(jnp.bfloat16)).astype(jnp.float32)
    blocked_values = values_head.astype(jnp.float32).reshape(seq_count, N_KV, POS_DEV, HEAD_DIM)
    sums = jnp.einsum('snt,sntd->snd', rounded, blocked_values)
    peak = jnp.maximum(lax.optimization_barrier(jnp.max(maxima, axis=1)), score_new)
    block_weight = jnp.exp(maxima - peak[:, None])
    new_weight = jnp.exp(score_new - peak)
    denominator = lax.optimization_barrier(jnp.sum(block_weight * totals, axis=1)) + new_weight
    numerator = lax.optimization_barrier(jnp.sum(block_weight[:, :, None] * sums, axis=1)) + new_weight[:, None] * value_new.astype(jnp.float32)
    return numerator / denominator[:, None]

def grouped_product(activations, weights_mat, groups):
    span_rows = weights_mat.shape[0] // groups
    result = jnp.zeros((activations.shape[0], weights_mat.shape[1]), jnp.float32)
    for block_index in range(groups):
        partial_value = jnp.dot(activations[:, block_index * span_rows:(block_index + 1) * span_rows], weights_mat[block_index * span_rows:(block_index + 1) * span_rows], preferred_element_type=jnp.float32)
        result = result + lax.optimization_barrier(partial_value.astype(jnp.bfloat16)).astype(jnp.float32)
    return result

def reference(tokens, attn_gain, w_query, w_key, w_value, cache_keys, cache_values, lambdas, head_gain, w_out, mlp_gain, w_gate, w_up, w_down):
    seq_count = tokens.shape[0]
    tokens_f = tokens.astype(jnp.float32)
    scale_in = lax.rsqrt(lax.optimization_barrier(jnp.mean(tokens_f * tokens_f, axis=1, keepdims=True)) + epsilon)
    normed_in = (tokens_f * attn_gain.astype(jnp.float32)).astype(jnp.bfloat16)

    def project(weight):
        product = jnp.dot(normed_in, weight, preferred_element_type=jnp.float32)
        return (scale_in * product).astype(jnp.bfloat16).reshape(seq_count, HEADS, HEAD_DIM)
    query_all = project(w_query)
    key_all = project(w_key)
    value_all = project(w_value)

    def one_head(head_index):
        keys_head = lax.dynamic_index_in_dim(cache_keys, head_index, 2, keepdims=False)
        values_head = lax.dynamic_index_in_dim(cache_values, head_index, 2, keepdims=False)
        query_vec = lax.dynamic_index_in_dim(query_all, head_index, 1, keepdims=False)
        key_new = lax.dynamic_index_in_dim(key_all, head_index, 1, keepdims=False)
        value_new = lax.dynamic_index_in_dim(value_all, head_index, 1, keepdims=False)
        first_map = blocked_attention(query_vec, key_new, value_new, keys_head, values_head, 0, HALF)
        second_map = blocked_attention(query_vec, key_new, value_new, keys_head, values_head, HALF, HEAD_DIM)
        return (first_map, second_map)
    first_map, second_map = lax.map(one_head, jnp.arange(HEADS, dtype=jnp.int32))
    difference = first_map - lambdas.astype(jnp.float32)[:, None, None] * second_map
    normed = difference * lax.rsqrt(lax.optimization_barrier(jnp.mean(difference * difference, axis=2, keepdims=True)) + epsilon)
    normed = normed * head_gain.astype(jnp.float32)
    heads_out = jnp.transpose(normed, (1, 0, 2)).reshape(seq_count, HEADS * HEAD_DIM).astype(jnp.bfloat16)
    branch = grouped_product(heads_out, w_out, N_TP)
    residual = (tokens_f + branch).astype(jnp.bfloat16)
    residual_f = residual.astype(jnp.float32)
    scale_mid = lax.rsqrt(lax.optimization_barrier(jnp.mean(residual_f * residual_f, axis=1, keepdims=True)) + epsilon)
    normed_mid = (residual_f * mlp_gain.astype(jnp.float32)).astype(jnp.bfloat16)
    gate = scale_mid * jnp.dot(normed_mid, w_gate, preferred_element_type=jnp.float32)
    up_val = scale_mid * jnp.dot(normed_mid, w_up, preferred_element_type=jnp.float32)
    hidden = (jax.nn.silu(gate) * up_val).astype(jnp.bfloat16)
    mixer = grouped_product(hidden, w_down, N_TP)
    return (residual_f + mixer).astype(jnp.bfloat16)
```

```python
import functools

import jax
import jax.numpy as jnp
from jax import lax
from jax.experimental import pallas as pl
from jax.experimental.pallas import tpu as pltpu
from jax.sharding import PartitionSpec as P

epsilon = 1e-06
MESH = pl.DeviceIdType.MESH
F32 = jnp.float32
BF16 = jnp.bfloat16
Q_LINK = jnp.bfloat16
KV_LINK = jnp.float32
FF_LINK = jnp.bfloat16


def partner(me, step, count):
    if count & (count - 1):
        return lax.rem(me + step, count)
    peer, bit = 0, 1
    while bit < count:
        digit = lax.rem(lax.div(me, bit), 2)
        peer = peer + bit * (1 - digit if step & bit else digit)
        bit *= 2
    return peer


def sender(me, step, count):
    if count & (count - 1):
        return lax.rem(me + count - step, count)
    return partner(me, step, count)


def peers(axis, count):
    me = lax.axis_index(axis)
    return [(step, partner(me, step, count)) for step in reversed(range(1, count))]


def exchange(axis, count, source, target, send_sem, recv_sem):
    copies = []
    for step, peer in peers(axis, count):
        copy = pltpu.make_async_remote_copy(
            src_ref=source(peer),
            dst_ref=target,
            send_sem=send_sem.at[step - 1],
            recv_sem=recv_sem.at[step - 1],
            device_id={axis: peer},
            device_id_type=MESH,
        )
        copy.start()
        copies.append(copy)
    return copies


def to_row(column):
    rows = column.shape[0]
    spot = lax.broadcasted_iota(jnp.int32, (rows, 128), 0) == lax.broadcasted_iota(
        jnp.int32, (rows, 128), 1
    )
    return jnp.sum(jnp.where(spot, column, 0.0), axis=0, keepdims=True)


def to_column(row, rows):
    spot = lax.broadcasted_iota(jnp.int32, (rows, 128), 0) == lax.broadcasted_iota(
        jnp.int32, (rows, 128), 1
    )
    return jnp.sum(jnp.where(spot, row, 0.0), axis=1, keepdims=True)


def wait_recv(copies):
    for copy in copies:
        copy.wait_recv()


def wait_send(copies):
    for copy in copies:
        copy.wait_send()


def pad_rows(value, rows):
    if value.shape[0] == rows:
        return value
    return jnp.concatenate(
        [value, jnp.zeros((rows - value.shape[0],) + value.shape[1:], value.dtype)], axis=0
    )


def pad_cols(value, cols):
    if value.shape[1] == cols:
        return value
    return jnp.concatenate(
        [value, jnp.zeros((value.shape[0], cols - value.shape[1]), value.dtype)], axis=1
    )


def layer_kernel(
    dims, tok_in, gain_in, wq_in, wk_in, wv_in, keys_in, values_in, lam_in, head_gain_in, w_out_in,
    mid_gain_in, w_gate_in, w_up_in, w_down_in,
    out,
    tok, gain, lam, head_gain, mid_gain, wq, wk, wv, keys, values, wo, wg, wu, wd,
    tok_all, sq_all, q_part, q_got, q_own, q_all, kv_part, kv_got, q_seq, scores, acc, lse,
    o_in, o_all, l_in, l_all, h_own, h_all, b_all, mid_all, gu_part, gu_all, hid_own, hid_all,
    d_part, d_all,
    w_sem, k_sem, v_sem, *sems,
):
    n_kv, n_tp, groups, rows, width, chunk, per_step = dims
    seqs, own = out.shape
    heads = n_kv // groups
    hubs, first = n_kv // 2, n_kv // 4
    hd = head_gain.shape[1]
    half_dim = hd // 2
    score_scale = half_dim ** (-0.5)
    length = keys.shape[1]
    steps = seqs // per_step
    pairs = [(sems[2 * at], sems[2 * at + 1]) for at in range(len(sems) // 2)]
    t_sem, b_sem, d_sem = pairs[:3]
    sq_sem, m_sem, q_sem, kv_sem, o_sem, l_sem, g_sem = pairs[3:10]
    qa_sem, h_sem, i_sem = pairs[10:13]

    def load(index, source, target):
        copy = pltpu.make_async_copy(source, target, w_sem.at[index])
        copy.start()
        return copy

    load_tok = load(0, tok_in, tok)
    load_gain = load(1, gain_in, gain)
    load_q = load(2, wq_in, wq)
    load_k = load(3, wk_in, wk)
    load_v = load(4, wv_in, wv)

    def cache_copies(step):
        at = pl.ds(step * per_step, per_step)
        return (
            pltpu.make_async_copy(keys_in.at[at], keys.at[at], k_sem.at[step]),
            pltpu.make_async_copy(values_in.at[at], values.at[at], v_sem.at[step]),
        )

    for step in range(steps):
        for copy in cache_copies(step):
            copy.start()
    load_lam = load(5, lam_in, lam)
    load_hg = load(6, head_gain_in, head_gain)
    load_mg = load(7, mid_gain_in, mid_gain)
    load_wo = load(8, w_out_in, wo)
    units = w_down_in.shape[0]
    load_wg = load(9, w_gate_in, wg.at[pl.ds(0, units)])
    load_wu = load(10, w_up_in, wu.at[pl.ds(0, units)])
    load_wd = load(11, w_down_in, wd.at[pl.ds(0, units)])
    if units < hubs * chunk:
        for buf in (wg, wu, wd):
            buf[units:, :] = jnp.zeros((hubs * chunk - units, buf.shape[1]), BF16)

    me = lax.axis_index("kv")
    me_tp = lax.axis_index("tp")
    side = lax.rem(me_tp, 2)
    lead = me_tp + 1 - side
    spot = me - first
    low = 1 - lax.div(me, hubs)
    is_hub = (side == 1) & (me >= first) & (me < first + hubs)
    far_first = [s + low * (hubs - 1 - 2 * s) for s in range(hubs)]
    sent = []

    def hub_at(hub):
        return {"kv": first + hub, "tp": lead}

    def at_home(hub):
        return (side == 1) & (first + hub == me)

    barrier = pltpu.get_barrier_semaphore()

    def greet(device):
        pl.semaphore_signal(barrier, inc=1, device_id=device, device_id_type=MESH)

    for _, peer in peers("tp", n_tp):
        greet({"kv": me, "tp": peer})
    for hub in far_first:
        pl.when(jnp.logical_not(at_home(hub)))(functools.partial(greet, hub_at(hub)))

    @pl.when(is_hub)
    def _():
        for step in reversed(range(n_kv)):
            for part in range(2):
                if step > 0 or part == 0:
                    greet({"kv": partner(me, step, n_kv), "tp": me_tp - 1 + part})
        pl.semaphore_wait(barrier, n_tp - 1 + 2 * n_kv - 1 + hubs - 1)

    @pl.when(jnp.logical_not(is_hub))
    def _():
        pl.semaphore_wait(barrier, n_tp - 1 + hubs)

    def to_hub(hub, s, source, target, sem):
        home = at_home(hub)
        copy = pltpu.make_async_remote_copy(
            src_ref=source,
            dst_ref=target.at[side, me],
            send_sem=sem[0].at[s],
            recv_sem=sem[1].at[side, me],
            device_id=hub_at(hub),
            device_id_type=MESH,
        )
        away = jnp.logical_not(home)
        pl.when(away)(copy.start)

        @pl.when(home)
        def _():
            target[1, me] = source[...]

        sent.append((away, copy))

    def to_hubs(source, target, sem):
        for s, hub in enumerate(far_first):
            to_hub(hub, s, source.at[hub], target, sem)

    def collected(target, sem, part):
        for step in range(part, n_kv):
            peer = sender(me, step, n_kv)
            pltpu.make_async_remote_copy(
                src_ref=target.at[part, peer],
                dst_ref=target.at[part, peer],
                send_sem=sem[0].at[0],
                recv_sem=sem[1].at[part, peer],
                device_id=hub_at(0),
                device_id_type=MESH,
            ).wait_recv()

    def row_copy(hub, s, target, sem):
        return pltpu.make_async_remote_copy(
            src_ref=target.at[me],
            dst_ref=target.at[me],
            send_sem=sem[0].at[s],
            recv_sem=sem[1].at[me],
            device_id=hub_at(hub),
            device_id_type=MESH,
        )

    def rows_to_hubs(target, sem):
        for s, hub in enumerate(far_first):
            away = (side == 1) & jnp.logical_not(at_home(hub))
            copy = row_copy(hub, s, target, sem)
            pl.when(away)(copy.start)
            sent.append((away, copy))

    def row_sum(target, sem):
        for step in range(1, n_kv):
            peer = sender(me, step, n_kv)
            pltpu.make_async_remote_copy(
                src_ref=target.at[peer],
                dst_ref=target.at[peer],
                send_sem=sem[0].at[0],
                recv_sem=sem[1].at[peer],
                device_id=hub_at(0),
                device_id_type=MESH,
            ).wait_recv()
        total = target[0]
        for index in range(1, n_kv):
            total = total + target[index]
        return lax.rsqrt(to_column(total, seqs) / width + epsilon)

    def spread_copy(part, step, source, target, sem):
        return pltpu.make_async_remote_copy(
            src_ref=source.at[part],
            dst_ref=target.at[spot],
            send_sem=sem[0].at[part, step],
            recv_sem=sem[1].at[spot],
            device_id={"kv": partner(me, step, n_kv), "tp": me_tp - 1 + part},
            device_id_type=MESH,
        )

    def spread(part, source, target, sem):
        for step in reversed(range(part, n_kv)):
            spread_copy(part, step, source, target, sem).start()
        if part == 1:
            target[spot] = source[1]

    def arrived(hub, target, sem):
        copy = pltpu.make_async_remote_copy(
            src_ref=target.at[hub],
            dst_ref=target.at[hub],
            send_sem=sem[0].at[0, 0],
            recv_sem=sem[1].at[hub],
            device_id=hub_at(0),
            device_id_type=MESH,
        )
        pl.when(jnp.logical_not(at_home(hub)))(copy.wait_recv)

    load_tok.wait()
    tok_copies = exchange("tp", n_tp, lambda peer: tok, tok_all.at[me_tp], *t_sem)
    tok_all[me_tp] = tok[...]
    load_gain.wait()
    wait_recv(tok_copies)
    xf = jnp.concatenate([tok_all[index] for index in range(n_tp)], axis=1).astype(F32)
    normed = (xf * gain[...]).astype(BF16)

    def project(buf, link):
        product = jnp.dot(normed, buf[...], preferred_element_type=F32).astype(link)
        product = pad_rows(product, groups * rows)
        return [
            product[group * rows : (group + 1) * rows, head * hd : (head + 1) * hd]
            for head in range(heads)
            for group in range(groups)
        ]

    def piece_rows(column, index):
        if groups == 1:
            return column
        column = pad_rows(column, groups * rows)
        group_of = lax.rem(2 * spot + index, groups)
        mine = column[:rows]
        for group in range(1, groups):
            mine = jnp.where(group_of == group, column[group * rows : (group + 1) * rows], mine)
        return mine

    load_q.wait()
    for piece, value in enumerate(project(wq, Q_LINK)):
        q_part[piece // 2, piece % 2] = value
    to_hubs(q_part, q_got, q_sem)
    sq_all[me] = to_row(jnp.sum(xf * xf, axis=1, keepdims=True))
    rows_to_hubs(sq_all, sq_sem)
    load_k.wait()
    for piece, value in enumerate(project(wk, KV_LINK)):
        kv_part[piece // 2, piece % 2, 0] = value
    load_v.wait()
    for piece, value in enumerate(project(wv, KV_LINK)):
        kv_part[piece // 2, piece % 2, 1] = value

    @pl.when(is_hub)
    def _():
        scale = row_sum(sq_all, sq_sem)
        for part in (1, 0):
            collected(q_got, q_sem, part)
            for index in range(2):
                total = q_got[part, 0, index].astype(F32)
                for source in range(1, n_kv):
                    total = total + q_got[part, source, index].astype(F32)
                q_own[part, index] = (piece_rows(scale, index) * total).astype(BF16)
            spread(part, q_own, q_all, qa_sem)

    for hub in range(hubs):
        arrived(hub, q_all, qa_sem)
    to_hubs(kv_part, kv_got, kv_sem)
    for piece in range(n_kv):
        head, group = piece // groups, piece % groups
        q_seq[group * rows : (group + 1) * rows, head : head + 1, :] = q_all[
            piece // 2, piece % 2
        ].astype(F32)[:, None, :]

    row = lax.broadcasted_iota(jnp.int32, (2 * heads * per_step, length), 0)
    col = lax.broadcasted_iota(jnp.int32, (2 * heads * per_step, length), 1)
    keep = lax.rem(col, heads) == lax.rem(row, heads)
    stat_lane = lax.broadcasted_iota(jnp.int32, (2 * heads, 128), 1)
    q_lane = lax.broadcasted_iota(jnp.int32, (heads, hd), 1)
    lse[...] = jnp.zeros_like(lse)

    def queries(seq):
        vec = q_seq[seq]
        return jnp.concatenate(
            [jnp.where(q_lane < half_dim, vec, 0.0), jnp.where(q_lane < half_dim, 0.0, vec)],
            axis=0,
        ).astype(BF16)

    def wide(parts):
        return parts[0] if per_step == 1 else jnp.concatenate(parts, axis=1)

    def score(at):
        span = range(at * per_step, (at + 1) * per_step)
        blank = jnp.zeros((2 * heads, hd), BF16)
        query = jnp.concatenate(
            [wide([queries(seq) if other == seq else blank for other in span]) for seq in span],
            axis=0,
        )
        scores[at % 2] = lax.dot_general(
            query, wide([keys[seq] for seq in span]), (((1,), (1,)), ((), ())),
            preferred_element_type=F32,
        )

    def attend(at):
        span = range(at * per_step, (at + 1) * per_step)
        level = jnp.where(keep, scores[at % 2] * score_scale, -jnp.inf)
        peak = jnp.max(level, axis=1, keepdims=True)
        weights = jnp.exp(level - peak)
        total = jnp.sum(weights, axis=1, keepdims=True)
        summed = jnp.dot(
            weights.astype(BF16), wide([values[seq] for seq in span]), preferred_element_type=F32
        )
        result = summed / total
        level = peak + jnp.log(total)
        stats = lse[...]
        for index, seq in enumerate(span):
            part = slice(index * 2 * heads, (index + 1) * 2 * heads)
            acc[:, seq : seq + 1, :] = result[part, index * hd : (index + 1) * hd][:, None, :]
            stats = jnp.where(stat_lane == seq, level[part], stats)
        lse[...] = stats

    for step in range(steps):
        for copy in cache_copies(step):
            copy.wait()
    score(0)
    for step in range(steps):
        if step + 1 < steps:
            score(step + 1)
        attend(step)

    load_lam.wait()
    last_lane = lax.broadcasted_iota(jnp.int32, (1, 128), 1) == 127
    for piece in range(n_kv):
        head, group = piece // groups, piece % groups
        span = slice(group * rows, (group + 1) * rows)
        for half in range(2):
            at = half * heads + head
            o_in[piece // 2, piece % 2, half] = acc[at, span, :].astype(BF16)
            l_in[piece // 2, 2 * (piece % 2) + half : 2 * (piece % 2) + half + 1, :] = jnp.where(
                last_lane, lam[:, head : head + 1], pad_cols(lse[at : at + 1, span], 128)
            )
    to_hubs(l_in, l_all, l_sem)
    to_hubs(o_in, o_all, o_sem)
    load_hg.wait()
    load_mg.wait()

    @pl.when(is_hub)
    def _():
        total = sq_all[0]
        for index in range(1, n_kv):
            total = total + sq_all[index]
        scale = lax.rsqrt(to_column(total, seqs) / width + epsilon)
        lane = lax.broadcasted_iota(jnp.int32, (rows, hd), 1)
        fresh, value_new = {}, {}
        for part in (1, 0):
            collected(kv_got, kv_sem, part)
            for index in range(2):
                mine = piece_rows(scale, index)
                k_sum, v_sum = kv_got[part, 0, index, 0], kv_got[part, 0, index, 1]
                for source in range(1, n_kv):
                    k_sum = k_sum + kv_got[part, source, index, 0]
                    v_sum = v_sum + kv_got[part, source, index, 1]
                k_new = (mine * k_sum).astype(BF16).astype(F32)
                value_new[part, index] = (mine * v_sum).astype(BF16).astype(F32)
                product = q_own[part, index].astype(F32) * k_new
                for half in range(2):
                    inside = (lane < half_dim) if half == 0 else (lane >= half_dim)
                    fresh[part, index, half] = to_row(
                        jnp.sum(jnp.where(inside, product, 0.0), axis=1, keepdims=True)
                        * score_scale
                    )
        for part in (1, 0):
            collected(l_all, l_sem, part)
            shares = []
            for index in range(2):
                for half in range(2):
                    at = 2 * index + half
                    level = jnp.concatenate(
                        [l_all[part, source, at : at + 1, :] for source in range(n_kv)]
                        + [fresh[part, index, half]],
                        axis=0,
                    )
                    share = jnp.exp(level - jnp.max(level, axis=0, keepdims=True))
                    share = share / jnp.sum(share, axis=0, keepdims=True)
                    if half == 1:
                        share = share * -l_all[part, 0, at : at + 1, 127:]
                    shares.append(share)
            count = n_kv + 1
            columns = []
            for begin in range(0, 4, max(1, 128 // count)):
                block = jnp.concatenate(shares[begin : begin + max(1, 128 // count)], axis=0)
                turned = jnp.transpose(pad_rows(block, 128))
                columns += [
                    turned[:rows, at : at + 1] for at in range(block.shape[0])
                ]
            collected(o_all, o_sem, part)
            for index in range(2):
                difference = 0.0
                for half in range(2):
                    at = (2 * index + half) * count
                    top = columns[at + n_kv] * value_new[part, index]
                    for source in range(n_kv):
                        top = top + columns[at + source] * o_all[part, source, index, half].astype(
                            F32
                        )
                    difference = difference + top
                normal = (
                    difference
                    * lax.rsqrt(jnp.mean(difference * difference, axis=1, keepdims=True) + epsilon)
                    * head_gain[...]
                )
                h_own[part, index] = normal.astype(BF16)
            spread(part, h_own, h_all, h_sem)

    load_wo.wait()
    if groups == 1:
        shared = None
        for hub in reversed(far_first):
            arrived(hub, h_all, h_sem)
            share = jnp.dot(
                jnp.concatenate([h_all[hub, 0], h_all[hub, 1]], axis=1),
                wo[pl.ds(pl.multiple_of(hub * 2 * hd, 2 * hd), 2 * hd), :],
                preferred_element_type=F32,
            )
            shared = share if shared is None else shared + share
    else:
        for hub in range(hubs):
            arrived(hub, h_all, h_sem)
        columns = []
        for head in range(heads):
            pieces = range(head * groups, (head + 1) * groups)
            column = [h_all[piece // 2, piece % 2].astype(F32) for piece in pieces]
            columns.append(jnp.concatenate(column, axis=0)[:seqs].astype(BF16))
        shared = jnp.dot(
            jnp.concatenate(columns, axis=1), wo[...], preferred_element_type=F32
        )
    b_all[me_tp] = shared.astype(BF16)
    b_copies = exchange("tp", n_tp, lambda peer: b_all.at[me_tp], b_all.at[me_tp], *b_sem)
    wait_recv(b_copies)
    branch = b_all[0].astype(F32)
    for index in range(1, n_tp):
        branch = branch + b_all[index].astype(F32)
    residual = (xf + branch).astype(BF16)
    res_f = residual.astype(F32)
    normed_mid = (res_f * mid_gain[...]).astype(BF16)
    load_wg.wait()
    load_wu.wait()
    for s, hub in enumerate(far_first):
        at = pl.ds(pl.multiple_of(hub * chunk, 16), chunk)
        gu_part[s] = lax.dot_general(
            normed_mid, jnp.concatenate([wg[at, :], wu[at, :]], axis=0),
            (((1,), (1,)), ((), ())), preferred_element_type=F32,
        ).astype(FF_LINK)
        to_hub(hub, s, gu_part.at[s], gu_all, g_sem)
        if s == 0:
            mid_all[me] = to_row(jnp.sum(res_f * res_f, axis=1, keepdims=True))
            rows_to_hubs(mid_all, m_sem)

    @pl.when(is_hub)
    def _():
        scale = row_sum(mid_all, m_sem)
        for part in (1, 0):
            collected(gu_all, g_sem, part)
            total = gu_all[part, 0].astype(F32)
            for source in range(1, n_kv):
                total = total + gu_all[part, source].astype(F32)
            gate, up = scale * total[:, :chunk], scale * total[:, chunk:]
            hid_own[part] = (gate / (1.0 + jnp.exp(-gate)) * up).astype(BF16)
            spread(part, hid_own, hid_all, i_sem)

    load_wd.wait()
    down = None
    for hub in reversed(far_first):
        arrived(hub, hid_all, i_sem)
        share = jnp.dot(
            hid_all[hub],
            wd[pl.ds(pl.multiple_of(hub * chunk, 16), chunk), :],
            preferred_element_type=F32,
        )
        down = share if down is None else down + share
    down = down.astype(BF16)
    for index in range(n_tp):
        d_part[index] = down[:, index * own : (index + 1) * own]
    d_copies = exchange("tp", n_tp, lambda peer: d_part.at[peer], d_all.at[me_tp], *d_sem)
    d_all[me_tp] = d_part[me_tp]
    base = res_f[:, :own]
    for index in range(1, n_tp):
        base = jnp.where(me_tp == index, res_f[:, index * own : (index + 1) * own], base)
    wait_recv(d_copies)
    mixer = d_all[0].astype(F32)
    for index in range(1, n_tp):
        mixer = mixer + d_all[index].astype(F32)
    out[...] = (base + mixer).astype(BF16)
    wait_send(tok_copies + b_copies + d_copies)
    for away, copy in sent:
        pl.when(away)(copy.wait_send)

    @pl.when(is_hub)
    def _():
        for source, target, sem in (
            (q_own, q_all, qa_sem), (h_own, h_all, h_sem), (hid_own, hid_all, i_sem)
        ):
            for part in range(2):
                for step in range(part, n_kv):
                    spread_copy(part, step, source, target, sem).wait_send()


ANY = pl.BlockSpec(memory_space=pl.ANY)


def per_device(
    n_kv, n_tp, tokens, attn_gain, w_query, w_key, w_value, cache_keys, cache_values, lambdas,
    head_gain, w_out, mlp_gain, w_gate, w_up, w_down,
):
    seqs, own = tokens.shape
    heads = lambdas.shape[0]
    hd = head_gain.shape[0]
    feats = attn_gain.shape[0]
    width = feats * n_kv
    groups = n_kv // heads
    rows = -(-seqs // groups)
    units = w_gate.shape[1]
    hubs = n_kv // 2
    chunk = 16 * -(-units // (16 * hubs))
    length = cache_keys.shape[1] * heads
    per_step = 2 if seqs % 2 == 0 else 1
    dma = pltpu.SemaphoreType.DMA
    tp_sems = [dma((n_tp - 1,)), dma((n_tp - 1,))]
    row_sems = [dma((hubs,)), dma((n_kv,))]
    hub_sems = [dma((hubs,)), dma((2, n_kv))]
    out_sems = [dma((2, n_kv)), dma((hubs,))]
    vm = pltpu.VMEM
    return pl.pallas_call(
        functools.partial(layer_kernel, (n_kv, n_tp, groups, rows, width, chunk, per_step)),
        out_shape=pltpu.VMEM((seqs, own), BF16),
        in_specs=[ANY] * 14,
        out_specs=pl.BlockSpec(memory_space=pltpu.VMEM),
        scratch_shapes=[
            vm((seqs, own), BF16),
            vm((1, feats), F32),
            vm((1, heads), F32),
            vm((1, hd), F32),
            vm((1, feats), F32),
            vm(w_query.shape, BF16),
            vm(w_key.shape, BF16),
            vm(w_value.shape, BF16),
            vm((seqs, length, hd), BF16),
            vm((seqs, length, hd), BF16),
            vm(w_out.shape, BF16),
            vm((hubs * chunk, feats), BF16),
            vm((hubs * chunk, feats), BF16),
            vm((hubs * chunk, w_down.shape[1]), BF16),
            vm((n_tp, seqs, own), BF16),
            vm((n_kv, 1, 128), F32),
            vm((hubs, 2, rows, hd), Q_LINK),
            vm((2, n_kv, 2, rows, hd), Q_LINK),
            vm((2, 2, rows, hd), BF16),
            vm((hubs, 2, rows, hd), BF16),
            vm((hubs, 2, 2, rows, hd), KV_LINK),
            vm((2, n_kv, 2, 2, rows, hd), KV_LINK),
            vm((groups * rows, heads, hd), F32),
            vm((2, 2 * heads * per_step, length), F32),
            vm((2 * heads, groups * rows, hd), F32),
            vm((2 * heads, 128), F32),
            vm((hubs, 2, 2, rows, hd), BF16),
            vm((2, n_kv, 2, 2, rows, hd), BF16),
            vm((hubs, 4, 128), F32),
            vm((2, n_kv, 4, 128), F32),
            vm((2, 2, rows, hd), BF16),
            vm((hubs, 2, rows, hd), BF16),
            vm((n_tp, seqs, feats), BF16),
            vm((n_kv, 1, 128), F32),
            vm((hubs, seqs, 2 * chunk), FF_LINK),
            vm((2, n_kv, seqs, 2 * chunk), FF_LINK),
            vm((2, seqs, chunk), BF16),
            vm((hubs, seqs, chunk), BF16),
            vm((n_tp, seqs, own), BF16),
            vm((n_tp, seqs, own), BF16),
            dma((12,)), dma((seqs // per_step,)), dma((seqs // per_step,)),
            *(tp_sems * 3), *(row_sems * 2), *(hub_sems * 5), *(out_sems * 3),
        ],
        compiler_params=pltpu.CompilerParams(
            collective_id=0, has_side_effects=True, vmem_limit_bytes=62 << 20
        ),
        name="layer",
    )(
        tokens, attn_gain.reshape(1, feats), w_query, w_key, w_value,
        cache_keys.reshape(seqs, length, hd), cache_values.reshape(seqs, length, hd),
        lambdas.reshape(1, heads), head_gain.reshape(1, hd), w_out, mlp_gain.reshape(1, feats),
        w_gate.T, w_up.T, w_down,
    )


def solution(mesh):
    in_specs = (
        P(None, ("kv", "tp")), P("kv"), P("kv", "tp"), P("kv", "tp"), P("kv", "tp"),
        P(None, "kv", "tp", None), P(None, "kv", "tp", None), P("tp"), P(),
        P("tp", "kv"), P("kv"), P("kv", "tp"), P("kv", "tp"), P("tp", "kv"),
    )
    return jax.shard_map(
        functools.partial(per_device, mesh.shape["kv"], mesh.shape["tp"]),
        mesh=mesh, in_specs=in_specs, out_specs=P(None, ("kv", "tp")), check_vma=False,
    )
```

```python
import functools

import jax
import jax.numpy as jnp
from jax import lax
from jax.experimental import pallas as pl
from jax.experimental.pallas import tpu as pltpu
from jax.sharding import PartitionSpec as P

epsilon = 1e-06
MESH = pl.DeviceIdType.MESH
F32 = jnp.float32
BF16 = jnp.bfloat16
Q_LINK = jnp.bfloat16
KV_LINK = jnp.float32
FF_LINK = jnp.bfloat16


def partner(me, step, count):
    if count & (count - 1):
        return lax.rem(me + step, count)
    peer, bit = 0, 1
    while bit < count:
        digit = lax.rem(lax.div(me, bit), 2)
        peer = peer + bit * (1 - digit if step & bit else digit)
        bit *= 2
    return peer


def sender(me, step, count):
    if count & (count - 1):
        return lax.rem(me + count - step, count)
    return partner(me, step, count)


def peers(axis, count):
    me = lax.axis_index(axis)
    return [(step, partner(me, step, count)) for step in reversed(range(1, count))]


def exchange(axis, count, source, target, send_sem, recv_sem):
    copies = []
    for step, peer in peers(axis, count):
        copy = pltpu.make_async_remote_copy(
            src_ref=source(peer),
            dst_ref=target,
            send_sem=send_sem.at[step - 1],
            recv_sem=recv_sem.at[step - 1],
            device_id={axis: peer},
            device_id_type=MESH,
        )
        copy.start()
        copies.append(copy)
    return copies


def to_row(column):
    rows = column.shape[0]
    spot = lax.broadcasted_iota(jnp.int32, (rows, 128), 0) == lax.broadcasted_iota(
        jnp.int32, (rows, 128), 1
    )
    return jnp.sum(jnp.where(spot, column, 0.0), axis=0, keepdims=True)


def to_column(row, rows):
    spot = lax.broadcasted_iota(jnp.int32, (rows, 128), 0) == lax.broadcasted_iota(
        jnp.int32, (rows, 128), 1
    )
    return jnp.sum(jnp.where(spot, row, 0.0), axis=1, keepdims=True)


def wait_recv(copies):
    for copy in copies:
        copy.wait_recv()


def wait_send(copies):
    for copy in copies:
        copy.wait_send()


def pad_rows(value, rows):
    if value.shape[0] == rows:
        return value
    return jnp.concatenate(
        [value, jnp.zeros((rows - value.shape[0],) + value.shape[1:], value.dtype)], axis=0
    )


def pad_cols(value, cols):
    if value.shape[1] == cols:
        return value
    return jnp.concatenate(
        [value, jnp.zeros((value.shape[0], cols - value.shape[1]), value.dtype)], axis=1
    )


def layer_kernel(
    dims, tok_in, gain_in, wq_in, wk_in, wv_in, keys_in, values_in, lam_in, head_gain_in, w_out_in,
    mid_gain_in, w_gate_in, w_up_in, w_down_in,
    out,
    tok, gain, lam, head_gain, mid_gain, wq, wk, wv, keys, values, wo, wg, wu, wd,
    tok_all, sq_all, q_part, q_got, q_own, q_all, kv_part, kv_got, q_seq, scores, acc, lse,
    o_in, o_all, l_in, l_all, h_own, h_all, spread_w, b_all, mid_all, gu_part, gu_all, hid_own, hid_all,
    d_part, d_all,
    w_sem, k_sem, v_sem, *sems,
):
    n_kv, n_tp, groups, rows, width, chunk, per_step = dims
    seqs, own = out.shape
    heads = n_kv // groups
    hubs, first = n_kv // 2, n_kv // 4
    hd = head_gain.shape[1]
    half_dim = hd // 2
    score_scale = half_dim ** (-0.5)
    length = keys.shape[1]
    steps = seqs // per_step
    pairs = [(sems[2 * at], sems[2 * at + 1]) for at in range(len(sems) // 2)]
    t_sem, b_sem, d_sem = pairs[:3]
    sq_sem, m_sem, q_sem, kv_sem, o_sem, l_sem, g_sem = pairs[3:10]
    qa_sem, h_sem, i_sem = pairs[10:13]

    def load(index, source, target):
        copy = pltpu.make_async_copy(source, target, w_sem.at[index])
        copy.start()
        return copy

    load_tok = load(0, tok_in, tok)
    load_gain = load(1, gain_in, gain)
    load_q = load(2, wq_in, wq)
    load_k = load(3, wk_in, wk)
    load_v = load(4, wv_in, wv)

    def cache_copies(step):
        at = pl.ds(step * per_step, per_step)
        return (
            pltpu.make_async_copy(keys_in.at[at], keys.at[at], k_sem.at[step]),
            pltpu.make_async_copy(values_in.at[at], values.at[at], v_sem.at[step]),
        )

    for step in range(steps):
        for copy in cache_copies(step):
            copy.start()
    load_lam = load(5, lam_in, lam)
    load_hg = load(6, head_gain_in, head_gain)
    load_mg = load(7, mid_gain_in, mid_gain)
    load_wo = load(8, w_out_in, wo)
    units = w_down_in.shape[0]
    load_wg = load(9, w_gate_in, wg.at[pl.ds(0, units)])
    load_wu = load(10, w_up_in, wu.at[pl.ds(0, units)])
    load_wd = load(11, w_down_in, wd.at[pl.ds(0, units)])
    if units < hubs * chunk:
        for buf in (wg, wu, wd):
            buf[units:, :] = jnp.zeros((hubs * chunk - units, buf.shape[1]), BF16)

    me = lax.axis_index("kv")
    me_tp = lax.axis_index("tp")
    side = lax.rem(me_tp, 2)
    lead = me_tp + 1 - side
    spot = me - first
    low = 1 - lax.div(me, hubs)
    is_hub = (side == 1) & (me >= first) & (me < first + hubs)
    far_first = [s + low * (hubs - 1 - 2 * s) for s in range(hubs)]
    sent = []

    def hub_at(hub):
        return {"kv": first + hub, "tp": lead}

    def at_home(hub):
        return (side == 1) & (first + hub == me)

    barrier = pltpu.get_barrier_semaphore()

    def greet(device):
        pl.semaphore_signal(barrier, inc=1, device_id=device, device_id_type=MESH)

    for _, peer in peers("tp", n_tp):
        greet({"kv": me, "tp": peer})
    for hub in far_first:
        pl.when(jnp.logical_not(at_home(hub)))(functools.partial(greet, hub_at(hub)))

    @pl.when(is_hub)
    def _():
        for step in reversed(range(n_kv)):
            for part in range(2):
                if step > 0 or part == 0:
                    greet({"kv": partner(me, step, n_kv), "tp": me_tp - 1 + part})
        pl.semaphore_wait(barrier, n_tp - 1 + 2 * n_kv - 1 + hubs - 1)

    @pl.when(jnp.logical_not(is_hub))
    def _():
        pl.semaphore_wait(barrier, n_tp - 1 + hubs)

    def to_hub(hub, s, source, target, sem, late=None):
        home = at_home(hub)
        copy = pltpu.make_async_remote_copy(
            src_ref=source,
            dst_ref=target.at[side, me],
            send_sem=sem[0].at[s],
            recv_sem=sem[1].at[side, me],
            device_id=hub_at(hub),
            device_id_type=MESH,
        )
        away = jnp.logical_not(home)
        if late is None:
            pl.when(away)(copy.start)
        else:
            pl.when(away & (side != 0))(copy.start)
            late.append((away & (side == 0), copy))

        @pl.when(home)
        def _():
            target[1, me] = source[...]

        sent.append((away, copy))

    def to_hubs(source, target, sem):
        for s, hub in enumerate(far_first):
            to_hub(hub, s, source.at[hub], target, sem)

    def collected(target, sem, part):
        for step in range(part, n_kv):
            peer = sender(me, step, n_kv)
            pltpu.make_async_remote_copy(
                src_ref=target.at[part, peer],
                dst_ref=target.at[part, peer],
                send_sem=sem[0].at[0],
                recv_sem=sem[1].at[part, peer],
                device_id=hub_at(0),
                device_id_type=MESH,
            ).wait_recv()

    def row_copy(hub, s, target, sem):
        return pltpu.make_async_remote_copy(
            src_ref=target.at[me],
            dst_ref=target.at[me],
            send_sem=sem[0].at[s],
            recv_sem=sem[1].at[me],
            device_id=hub_at(hub),
            device_id_type=MESH,
        )

    def rows_to_hubs(target, sem):
        for s, hub in enumerate(far_first):
            away = (side == 1) & jnp.logical_not(at_home(hub))
            copy = row_copy(hub, s, target, sem)
            pl.when(away)(copy.start)
            sent.append((away, copy))

    def row_sum(target, sem):
        for step in range(1, n_kv):
            peer = sender(me, step, n_kv)
            pltpu.make_async_remote_copy(
                src_ref=target.at[peer],
                dst_ref=target.at[peer],
                send_sem=sem[0].at[0],
                recv_sem=sem[1].at[peer],
                device_id=hub_at(0),
                device_id_type=MESH,
            ).wait_recv()
        total = target[0]
        for index in range(1, n_kv):
            total = total + target[index]
        return lax.rsqrt(to_column(total, seqs) / width + epsilon)

    def spread_copy(part, step, source, target, sem):
        return pltpu.make_async_remote_copy(
            src_ref=source.at[part],
            dst_ref=target.at[spot],
            send_sem=sem[0].at[part, step],
            recv_sem=sem[1].at[spot],
            device_id={"kv": partner(me, step, n_kv), "tp": me_tp - 1 + part},
            device_id_type=MESH,
        )

    def spread(part, source, target, sem):
        for step in reversed(range(part, n_kv)):
            spread_copy(part, step, source, target, sem).start()
        if part == 1:
            target[spot] = source[1]

    def arrived(hub, target, sem):
        copy = pltpu.make_async_remote_copy(
            src_ref=target.at[hub],
            dst_ref=target.at[hub],
            send_sem=sem[0].at[0, 0],
            recv_sem=sem[1].at[hub],
            device_id=hub_at(0),
            device_id_type=MESH,
        )
        pl.when(jnp.logical_not(at_home(hub)))(copy.wait_recv)

    load_tok.wait()
    tok_copies = exchange("tp", n_tp, lambda peer: tok, tok_all.at[me_tp], *t_sem)
    tok_all[me_tp] = tok[...]
    load_gain.wait()
    tok_order = [(None, me_tp)] + [
        (copy, partner(me_tp, n_tp - 1 - at, n_tp)) for at, copy in reversed(list(enumerate(tok_copies)))
    ]
    by_part = own % 128 == 0
    q_product = None
    if by_part:
        load_q.wait()
        for order in range(n_tp):
            peer = tok_order[order][1]
            if order > 0:
                tok_order[order][0].wait_recv()
            at = pl.ds(pl.multiple_of(peer * own, own), own)
            share = jnp.dot(
                (tok_all[peer].astype(F32) * gain[:, at]).astype(BF16), wq[at, :],
                preferred_element_type=F32,
            )
            q_product = share if q_product is None else q_product + share
    else:
        wait_recv(tok_copies)
    xf = jnp.concatenate([tok_all[index] for index in range(n_tp)], axis=1).astype(F32)
    normed = (xf * gain[...]).astype(BF16)

    def project(buf, link, product=None):
        if product is None:
            product = jnp.dot(normed, buf[...], preferred_element_type=F32)
        product = pad_rows(product.astype(link), groups * rows)
        return [
            product[group * rows : (group + 1) * rows, head * hd : (head + 1) * hd]
            for head in range(heads)
            for group in range(groups)
        ]

    def piece_rows(column, index):
        if groups == 1:
            return column
        column = pad_rows(column, groups * rows)
        group_of = lax.rem(2 * spot + index, groups)
        mine = column[:rows]
        for group in range(1, groups):
            mine = jnp.where(group_of == group, column[group * rows : (group + 1) * rows], mine)
        return mine

    if not by_part:
        load_q.wait()
    for piece, value in enumerate(project(wq, Q_LINK, q_product)):
        q_part[piece // 2, piece % 2] = value
    to_hubs(q_part, q_got, q_sem)
    sq_all[me] = to_row(jnp.sum(xf * xf, axis=1, keepdims=True))
    rows_to_hubs(sq_all, sq_sem)
    load_k.wait()
    for piece, value in enumerate(project(wk, KV_LINK)):
        kv_part[piece // 2, piece % 2, 0] = value
    load_v.wait()
    for piece, value in enumerate(project(wv, KV_LINK)):
        kv_part[piece // 2, piece % 2, 1] = value

    @pl.when(is_hub)
    def _():
        scale = row_sum(sq_all, sq_sem)
        for part in (1, 0):
            collected(q_got, q_sem, part)
            for index in range(2):
                total = q_got[part, 0, index].astype(F32)
                for source in range(1, n_kv):
                    total = total + q_got[part, source, index].astype(F32)
                q_own[part, index] = (piece_rows(scale, index) * total).astype(BF16)
            spread(part, q_own, q_all, qa_sem)

    for hub in range(hubs):
        arrived(hub, q_all, qa_sem)
    to_hubs(kv_part, kv_got, kv_sem)
    for piece in range(n_kv):
        head, group = piece // groups, piece % groups
        q_seq[group * rows : (group + 1) * rows, head : head + 1, :] = q_all[
            piece // 2, piece % 2
        ].astype(F32)[:, None, :]

    row = lax.broadcasted_iota(jnp.int32, (2 * heads * per_step, length), 0)
    col = lax.broadcasted_iota(jnp.int32, (2 * heads * per_step, length), 1)
    keep = lax.rem(col, heads) == lax.rem(row, heads)
    stat_lane = lax.broadcasted_iota(jnp.int32, (2 * heads, 128), 1)
    q_lane = lax.broadcasted_iota(jnp.int32, (heads, hd), 1)
    lse[...] = jnp.zeros_like(lse)

    def queries(seq):
        vec = q_seq[seq]
        return jnp.concatenate(
            [jnp.where(q_lane < half_dim, vec, 0.0), jnp.where(q_lane < half_dim, 0.0, vec)],
            axis=0,
        ).astype(BF16)

    def wide(parts):
        return parts[0] if per_step == 1 else jnp.concatenate(parts, axis=1)

    def score(at):
        span = range(at * per_step, (at + 1) * per_step)
        blank = jnp.zeros((2 * heads, hd), BF16)
        query = jnp.concatenate(
            [wide([queries(seq) if other == seq else blank for other in span]) for seq in span],
            axis=0,
        )
        scores[at % 2] = lax.dot_general(
            query, wide([keys[seq] for seq in span]), (((1,), (1,)), ((), ())),
            preferred_element_type=F32,
        )

    def attend(at):
        span = range(at * per_step, (at + 1) * per_step)
        level = jnp.where(keep, scores[at % 2] * score_scale, -jnp.inf)
        peak = jnp.max(level, axis=1, keepdims=True)
        weights = jnp.exp(level - peak)
        total = jnp.sum(weights, axis=1, keepdims=True)
        summed = jnp.dot(
            weights.astype(BF16), wide([values[seq] for seq in span]), preferred_element_type=F32
        )
        result = summed / total
        level = peak + jnp.log(total)
        stats = lse[...]
        for index, seq in enumerate(span):
            part = slice(index * 2 * heads, (index + 1) * 2 * heads)
            acc[:, seq : seq + 1, :] = result[part, index * hd : (index + 1) * hd][:, None, :]
            stats = jnp.where(stat_lane == seq, level[part], stats)
        lse[...] = stats

    for step in range(steps):
        for copy in cache_copies(step):
            copy.wait()
    score(0)
    for step in range(steps):
        if step + 1 < steps:
            score(step + 1)
        attend(step)

    load_lam.wait()
    last_lane = lax.broadcasted_iota(jnp.int32, (1, 128), 1) == 127
    for piece in range(n_kv):
        head, group = piece // groups, piece % groups
        span = slice(group * rows, (group + 1) * rows)
        for half in range(2):
            at = half * heads + head
            o_in[piece // 2, piece % 2, half] = acc[at, span, :].astype(BF16)
            l_in[piece // 2, 2 * (piece % 2) + half : 2 * (piece % 2) + half + 1, :] = jnp.where(
                last_lane, lam[:, head : head + 1], pad_cols(lse[at : at + 1, span], 128)
            )
    to_hubs(l_in, l_all, l_sem)
    to_hubs(o_in, o_all, o_sem)
    load_hg.wait()
    load_mg.wait()

    @pl.when(is_hub)
    def _():
        total = sq_all[0]
        for index in range(1, n_kv):
            total = total + sq_all[index]
        scale = lax.rsqrt(to_column(total, seqs) / width + epsilon)
        lane = lax.broadcasted_iota(jnp.int32, (rows, hd), 1)
        fresh, value_new = {}, {}
        for part in (1, 0):
            collected(kv_got, kv_sem, part)
            for index in range(2):
                mine = piece_rows(scale, index)
                k_sum, v_sum = kv_got[part, 0, index, 0], kv_got[part, 0, index, 1]
                for source in range(1, n_kv):
                    k_sum = k_sum + kv_got[part, source, index, 0]
                    v_sum = v_sum + kv_got[part, source, index, 1]
                k_new = (mine * k_sum).astype(BF16).astype(F32)
                value_new[part, index] = (mine * v_sum).astype(BF16).astype(F32)
                product = q_own[part, index].astype(F32) * k_new
                for half in range(2):
                    inside = (lane < half_dim) if half == 0 else (lane >= half_dim)
                    fresh[part, index, half] = to_row(
                        jnp.sum(jnp.where(inside, product, 0.0), axis=1, keepdims=True)
                        * score_scale
                    )
        for part in (1, 0):
            collected(l_all, l_sem, part)
            shares = []
            for index in range(2):
                for half in range(2):
                    at = 2 * index + half
                    level = jnp.concatenate(
                        [l_all[part, source, at : at + 1, :] for source in range(n_kv)]
                        + [fresh[part, index, half]],
                        axis=0,
                    )
                    share = jnp.exp(level - jnp.max(level, axis=0, keepdims=True))
                    share = share / jnp.sum(share, axis=0, keepdims=True)
                    if half == 1:
                        share = share * -l_all[part, 0, at : at + 1, 127:]
                    shares.append(share)
            count = n_kv + 1
            at_column = 0
            for begin in range(0, 4, max(1, 128 // count)):
                block = jnp.concatenate(shares[begin : begin + max(1, 128 // count)], axis=0)
                turned = jnp.transpose(pad_rows(block, 128))
                for at in range(block.shape[0]):
                    spread_w[at_column] = jnp.broadcast_to(turned[:rows, at : at + 1], (rows, hd))
                    at_column += 1
            base_value = []
            for index in range(2):
                at = 2 * index * count + n_kv
                base_value.append(
                    (spread_w[at] + spread_w[at + count]) * value_new[part, index]
                )
            collected(o_all, o_sem, part)
            for index in range(2):
                tops = []
                for half in range(2):
                    at = (2 * index + half) * count
                    terms = [
                        spread_w[at + source] * o_all[part, source, index, half].astype(F32)
                        for source in range(n_kv)
                    ]
                    while len(terms) > 1:
                        terms = [
                            terms[i] + terms[i + 1] if i + 1 < len(terms) else terms[i]
                            for i in range(0, len(terms), 2)
                        ]
                    tops.append(terms[0])
                difference = base_value[index] + tops[0] + tops[1]
                normal = (
                    difference
                    * lax.rsqrt(jnp.mean(difference * difference, axis=1, keepdims=True) + epsilon)
                    * head_gain[...]
                )
                h_own[part, index] = normal.astype(BF16)
            spread(part, h_own, h_all, h_sem)

    load_wo.wait()
    if groups == 1:
        shared = None
        for hub in reversed(far_first):
            arrived(hub, h_all, h_sem)
            share = jnp.dot(
                jnp.concatenate([h_all[hub, 0], h_all[hub, 1]], axis=1),
                wo[pl.ds(pl.multiple_of(hub * 2 * hd, 2 * hd), 2 * hd), :],
                preferred_element_type=F32,
            )
            shared = share if shared is None else shared + share
    else:
        for hub in range(hubs):
            arrived(hub, h_all, h_sem)
        columns = []
        for head in range(heads):
            pieces = range(head * groups, (head + 1) * groups)
            column = [h_all[piece // 2, piece % 2].astype(F32) for piece in pieces]
            columns.append(jnp.concatenate(column, axis=0)[:seqs].astype(BF16))
        shared = jnp.dot(
            jnp.concatenate(columns, axis=1), wo[...], preferred_element_type=F32
        )
    b_all[me_tp] = shared.astype(BF16)
    b_copies = exchange("tp", n_tp, lambda peer: b_all.at[me_tp], b_all.at[me_tp], *b_sem)
    wait_recv(b_copies)
    branch = b_all[0].astype(F32)
    for index in range(1, n_tp):
        branch = branch + b_all[index].astype(F32)
    residual = (xf + branch).astype(BF16)
    res_f = residual.astype(F32)
    normed_mid = (res_f * mid_gain[...]).astype(BF16)
    load_wg.wait()
    load_wu.wait()
    late = []
    for s, hub in enumerate(far_first):
        at = pl.ds(pl.multiple_of(hub * chunk, 16), chunk)
        gu_part[s] = lax.dot_general(
            normed_mid, jnp.concatenate([wg[at, :], wu[at, :]], axis=0),
            (((1,), (1,)), ((), ())), preferred_element_type=F32,
        ).astype(FF_LINK)
        to_hub(hub, s, gu_part.at[s], gu_all, g_sem, late)
        if s == 0:
            mid_all[me] = to_row(jnp.sum(res_f * res_f, axis=1, keepdims=True))
            rows_to_hubs(mid_all, m_sem)

    for when, copy in late:
        pl.when(when)(copy.start)
    @pl.when(is_hub)
    def _():
        scale = row_sum(mid_all, m_sem)
        for part in (1, 0):
            collected(gu_all, g_sem, part)
            total = gu_all[part, 0].astype(F32)
            for source in range(1, n_kv):
                total = total + gu_all[part, source].astype(F32)
            gate, up = scale * total[:, :chunk], scale * total[:, chunk:]
            hid_own[part] = (gate / (1.0 + jnp.exp(-gate)) * up).astype(BF16)
            spread(part, hid_own, hid_all, i_sem)

    load_wd.wait()
    down = None
    for hub in reversed(far_first):
        arrived(hub, hid_all, i_sem)
        share = jnp.dot(
            hid_all[hub],
            wd[pl.ds(pl.multiple_of(hub * chunk, 16), chunk), :],
            preferred_element_type=F32,
        )
        down = share if down is None else down + share
    down = down.astype(BF16)
    for index in range(n_tp):
        d_part[index] = down[:, index * own : (index + 1) * own]
    d_copies = exchange("tp", n_tp, lambda peer: d_part.at[peer], d_all.at[me_tp], *d_sem)
    d_all[me_tp] = d_part[me_tp]
    base = res_f[:, :own]
    for index in range(1, n_tp):
        base = jnp.where(me_tp == index, res_f[:, index * own : (index + 1) * own], base)
    wait_recv(d_copies)
    mixer = d_all[0].astype(F32)
    for index in range(1, n_tp):
        mixer = mixer + d_all[index].astype(F32)
    out[...] = (base + mixer).astype(BF16)
    wait_send(tok_copies + b_copies + d_copies)
    for away, copy in sent:
        pl.when(away)(copy.wait_send)

    @pl.when(is_hub)
    def _():
        for source, target, sem in (
            (q_own, q_all, qa_sem), (h_own, h_all, h_sem), (hid_own, hid_all, i_sem)
        ):
            for part in range(2):
                for step in range(part, n_kv):
                    spread_copy(part, step, source, target, sem).wait_send()


ANY = pl.BlockSpec(memory_space=pl.ANY)


def per_device(
    n_kv, n_tp, tokens, attn_gain, w_query, w_key, w_value, cache_keys, cache_values, lambdas,
    head_gain, w_out, mlp_gain, w_gate, w_up, w_down,
):
    seqs, own = tokens.shape
    heads = lambdas.shape[0]
    hd = head_gain.shape[0]
    feats = attn_gain.shape[0]
    width = feats * n_kv
    groups = n_kv // heads
    rows = -(-seqs // groups)
    units = w_gate.shape[1]
    hubs = n_kv // 2
    chunk = 16 * -(-units // (16 * hubs))
    length = cache_keys.shape[1] * heads
    per_step = 2 if seqs % 2 == 0 else 1
    dma = pltpu.SemaphoreType.DMA
    tp_sems = [dma((n_tp - 1,)), dma((n_tp - 1,))]
    row_sems = [dma((hubs,)), dma((n_kv,))]
    hub_sems = [dma((hubs,)), dma((2, n_kv))]
    out_sems = [dma((2, n_kv)), dma((hubs,))]
    vm = pltpu.VMEM
    return pl.pallas_call(
        functools.partial(layer_kernel, (n_kv, n_tp, groups, rows, width, chunk, per_step)),
        out_shape=pltpu.VMEM((seqs, own), BF16),
        in_specs=[ANY] * 14,
        out_specs=pl.BlockSpec(memory_space=pltpu.VMEM),
        scratch_shapes=[
            vm((seqs, own), BF16),
            vm((1, feats), F32),
            vm((1, heads), F32),
            vm((1, hd), F32),
            vm((1, feats), F32),
            vm(w_query.shape, BF16),
            vm(w_key.shape, BF16),
            vm(w_value.shape, BF16),
            vm((seqs, length, hd), BF16),
            vm((seqs, length, hd), BF16),
            vm(w_out.shape, BF16),
            vm((hubs * chunk, feats), BF16),
            vm((hubs * chunk, feats), BF16),
            vm((hubs * chunk, w_down.shape[1]), BF16),
            vm((n_tp, seqs, own), BF16),
            vm((n_kv, 1, 128), F32),
            vm((hubs, 2, rows, hd), Q_LINK),
            vm((2, n_kv, 2, rows, hd), Q_LINK),
            vm((2, 2, rows, hd), BF16),
            vm((hubs, 2, rows, hd), BF16),
            vm((hubs, 2, 2, rows, hd), KV_LINK),
            vm((2, n_kv, 2, 2, rows, hd), KV_LINK),
            vm((groups * rows, heads, hd), F32),
            vm((2, 2 * heads * per_step, length), F32),
            vm((2 * heads, groups * rows, hd), F32),
            vm((2 * heads, 128), F32),
            vm((hubs, 2, 2, rows, hd), BF16),
            vm((2, n_kv, 2, 2, rows, hd), BF16),
            vm((hubs, 4, 128), F32),
            vm((2, n_kv, 4, 128), F32),
            vm((2, 2, rows, hd), BF16),
            vm((hubs, 2, rows, hd), BF16),
            vm((4 * (n_kv + 1), rows, hd), F32),
            vm((n_tp, seqs, feats), BF16),
            vm((n_kv, 1, 128), F32),
            vm((hubs, seqs, 2 * chunk), FF_LINK),
            vm((2, n_kv, seqs, 2 * chunk), FF_LINK),
            vm((2, seqs, chunk), BF16),
            vm((hubs, seqs, chunk), BF16),
            vm((n_tp, seqs, own), BF16),
            vm((n_tp, seqs, own), BF16),
            dma((12,)), dma((seqs // per_step,)), dma((seqs // per_step,)),
            *(tp_sems * 3), *(row_sems * 2), *(hub_sems * 5), *(out_sems * 3),
        ],
        compiler_params=pltpu.CompilerParams(
            collective_id=0, has_side_effects=True, vmem_limit_bytes=62 << 20
        ),
        name="layer",
    )(
        tokens, attn_gain.reshape(1, feats), w_query, w_key, w_value,
        cache_keys.reshape(seqs, length, hd), cache_values.reshape(seqs, length, hd),
        lambdas.reshape(1, heads), head_gain.reshape(1, hd), w_out, mlp_gain.reshape(1, feats),
        w_gate.T, w_up.T, w_down,
    )


def solution(mesh):
    in_specs = (
        P(None, ("kv", "tp")), P("kv"), P("kv", "tp"), P("kv", "tp"), P("kv", "tp"),
        P(None, "kv", "tp", None), P(None, "kv", "tp", None), P("tp"), P(),
        P("tp", "kv"), P("kv"), P("kv", "tp"), P("kv", "tp"), P("tp", "kv"),
    )
    return jax.shard_map(
        functools.partial(per_device, mesh.shape["kv"], mesh.shape["tp"]),
        mesh=mesh, in_specs=in_specs, out_specs=P(None, ("kv", "tp")), check_vma=False,
    )
```
